32 devices in a mesh: grp: 2 (over y), fs: 4 (over z), tp: 4 (over x, core).
Axes of the slice: x: 2, y: 2, z: 4, core: 2. Of those that a mesh axis runs over, the one named last changes fastest.
Arguments:
- stream_in: bfloat16 [3072, 2048], P(('grp', 'fs'), 'tp'), parts along dimension 0, may hold values from -6 to 6
- gain_before: bfloat16 [2048], P('tp'), may hold values from 0.099609375 to 1.8984375
- gain_mixer: bfloat16 [2048], P('tp'), may hold values from 0.099609375 to 1.8984375
- gain_after: bfloat16 [2048], P('tp'), may hold values from 0.099609375 to 1.8984375
- w_gate: bfloat16 [2048, 5632], P('fs', 'tp'), may hold values from -0.125 to 0.125
- w_upward: bfloat16 [2048, 5632], P('fs', 'tp'), may hold values from -0.125 to 0.125
- w_down: bfloat16 [5632, 2048], P('tp', 'fs'), may hold values from -0.078125 to 0.078125
- w_value: bfloat16 [2048, 1024], P('fs', 'tp'), may hold values from -0.125 to 0.125
- w_glu_gate: bfloat16 [2048, 1024], P('fs', 'tp'), may hold values from -0.125 to 0.125
- conv_taps: bfloat16 [31, 1024], P(None, 'tp'), may hold values from -1 to 1
- chan_gain: bfloat16 [1024], P('tp'), may hold values from 0.099609375 to 1.8984375
- chan_bias: bfloat16 [1024], P('tp'), may hold values from -3 to 3
- w_mix_out: bfloat16 [1024, 2048], P('tp', 'fs'), may hold values from -0.1875 to 0.1875
Outputs:
- stream_out: bfloat16 [3072, 2048], P(('grp', 'fs'), 'tp'), parts along dimension 0
The draws below stay inside these ranges and needn't reach their ends.
There are 2 independent parts, one for each index of `grp`. The reference program is written for one: setup_inputs(seed, part) draws one part's arguments, and reference() takes and returns one part's arrays. A program takes and returns all parts, laid end to end along the dimension named above; an argument that names none is the same for every part. Nothing has to cross between parts.
All inputs are finite; a program needn't handle non-finite values.
Results may differ from the reference program's by a relative error of at most 0.017.
Values may be sent and summed in bfloat16 or wider, within the bound.
A program may use at most 64 MiB of HBM per device.

```python
import jax
import jax.numpy as jnp
from jax import lax

D = 2048
FF = 5632
CHAN = 1024
KERNEL = 31
LEN = 128
TOKENS = 1536
N_TP = 4


def steps_of(rng, dims, split, low, high):
    loudness, own = 1.0, jax.random.fold_in(rng, 6)
    for dim, parts in split:
        draws = jnp.exp(jax.random.uniform(jax.random.fold_in(own, dim), (parts,), jnp.float32, low / len(split), high / len(split)))
        loudness = loudness * jnp.repeat(draws, dims[dim] // parts).reshape([-1 if axis == dim else 1 for axis in range(len(dims))])
    return loudness


def normal_values(own_key, dims, scale, limit, shards=(), kind=jnp.bfloat16):
    entries = scale * jax.random.normal(own_key, dims, jnp.float32)
    if shards:
        entries = entries * steps_of(own_key, dims, shards, -0.22, 0.18)
    return jnp.clip(entries, -limit, limit).astype(kind)


def setup_inputs(seed: int = 0, part: int = 0) -> dict:
    keys = jax.random.split(jax.random.key(seed), 14)
    part_keys = jax.random.split(jax.random.fold_in(keys[13], part), 14)
    stream_in = normal_values(part_keys[0], (TOKENS, D), 1.0, 6.0, ((0, 4), (1, 4)))
    gain_before = jnp.clip(1.0 + 0.18 * jax.random.normal(keys[1], (D,), jnp.float32), 0.099609375, 1.8984375).astype(jnp.bfloat16)
    gain_mixer = jnp.clip(1.0 + 0.18 * jax.random.normal(keys[2], (D,), jnp.float32), 0.099609375, 1.8984375).astype(jnp.bfloat16)
    gain_after = jnp.clip(1.0 + 0.18 * jax.random.normal(keys[3], (D,), jnp.float32), 0.099609375, 1.8984375).astype(jnp.bfloat16)
    w_gate = normal_values(keys[4], (D, FF), D ** -0.5, 0.125, ((0, 4), (1, 4)))
    w_upward = normal_values(keys[5], (D, FF), D ** -0.5, 0.125, ((0, 4), (1, 4)))
    w_down = normal_values(keys[6], (FF, D), FF ** -0.5, 0.078125, ((0, 4), (1, 4)))
    w_value = normal_values(keys[7], (D, CHAN), D ** -0.5, 0.125, ((0, 4), (1, 4)))
    w_glu_gate = normal_values(keys[8], (D, CHAN), D ** -0.5, 0.125, ((0, 4), (1, 4)))
    conv_taps = normal_values(keys[9], (KERNEL, CHAN), KERNEL ** -0.5, 1.0, ((1, 4),))
    chan_gain = jnp.clip(1.0 + 0.18 * jax.random.normal(keys[10], (CHAN,), jnp.float32), 0.099609375, 1.8984375).astype(jnp.bfloat16)
    chan_bias = normal_values(keys[11], (CHAN,), 0.5, 3.0, ((0, 4),))
    w_mix_out = normal_values(keys[12], (CHAN, D), CHAN ** -0.5, 0.1875, ((0, 4), (1, 4)))
    return dict(stream_in=stream_in, gain_before=gain_before, gain_mixer=gain_mixer, gain_after=gain_after, w_gate=w_gate, w_upward=w_upward, w_down=w_down, w_value=w_value, w_glu_gate=w_glu_gate, conv_taps=conv_taps, chan_gain=chan_gain, chan_bias=chan_bias, w_mix_out=w_mix_out)


epsilon = 1e-06

def rms_rows(stream, weights):
    values = stream.astype(jnp.float32)
    inverse = lax.rsqrt(lax.optimization_barrier(jnp.mean(values * values, axis=1, keepdims=True)) + epsilon)
    return (values * inverse * weights.astype(jnp.float32)).astype(jnp.bfloat16)

def shard_sums(left, right):
    width = left.shape[1] // N_TP

    def add_shard(running, number):
        operand = lax.dynamic_slice_in_dim(left, number * width, width, 1)
        factor = lax.dynamic_slice_in_dim(right, number * width, width, 0)
        partial_term = jnp.dot(operand, factor, preferred_element_type=jnp.float32).astype(jnp.bfloat16)
        partial_term = lax.optimization_barrier(partial_term)
        return (running + partial_term.astype(jnp.float32), None)
    initial = jnp.zeros((left.shape[0], right.shape[1]), jnp.float32)
    result, unused = lax.scan(add_shard, initial, jnp.arange(N_TP, dtype=jnp.int32))
    return result

def feed_forward(rows, w_gate, w_upward, w_down):
    gate = jnp.dot(rows, w_gate, preferred_element_type=jnp.float32)
    upward = jnp.dot(rows, w_upward, preferred_element_type=jnp.float32)
    hidden = (jax.nn.silu(gate) * upward).astype(jnp.bfloat16)
    return shard_sums(hidden, w_down)

def conv_module(rows, w_value, w_glu_gate, conv_taps, chan_gain, chan_bias, w_mix_out):
    value = jnp.dot(rows, w_value, preferred_element_type=jnp.float32)
    gating = jnp.dot(rows, w_glu_gate, preferred_element_type=jnp.float32)
    glued = value * jax.nn.sigmoid(gating)
    channels = glued.shape[1]
    grouped = glued.reshape(-1, LEN, channels)
    padded = jnp.pad(grouped, ((0, 0), (KERNEL - 1, 0), (0, 0)))
    taps = conv_taps.astype(jnp.float32)
    conv_sum = jnp.zeros_like(grouped)
    for lag_index in range(KERNEL):
        conv_sum = conv_sum + taps[lag_index] * padded[:, lag_index:lag_index + LEN]
    flat = conv_sum.reshape(-1, channels)
    average = lax.optimization_barrier(jnp.mean(flat, axis=1, keepdims=True))
    spread = lax.optimization_barrier(jnp.mean(flat * flat, axis=1, keepdims=True)) - average * average
    normed = (flat - average) * lax.rsqrt(spread + epsilon) * chan_gain.astype(jnp.float32) + chan_bias.astype(jnp.float32)
    mixed = jax.nn.silu(normed).astype(jnp.bfloat16)
    return shard_sums(mixed, w_mix_out)

def reference(stream_in, gain_before, gain_mixer, gain_after, w_gate, w_upward, w_down, w_value, w_glu_gate, conv_taps, chan_gain, chan_bias, w_mix_out):
    first = (stream_in.astype(jnp.float32) + 0.5 * feed_forward(rms_rows(stream_in, gain_before), w_gate, w_upward, w_down)).astype(jnp.bfloat16)
    branch = conv_module(rms_rows(first, gain_mixer), w_value, w_glu_gate, conv_taps, chan_gain, chan_bias, w_mix_out)
    second = (first.astype(jnp.float32) + branch).astype(jnp.bfloat16)
    third = second.astype(jnp.float32) + 0.5 * feed_forward(rms_rows(second, gain_after), w_gate, w_upward, w_down)
    return third.astype(jnp.bfloat16)
```

```python
import functools

import jax
import jax.numpy as jnp
from jax import lax
from jax.experimental import pallas as pl
from jax.experimental.pallas import tpu as pltpu
from jax.sharding import PartitionSpec as P

KERNEL = 31
LEN = 128
WIDE = 384
LEAD = 3
SUB = 16

epsilon = 1e-06
MESH = pl.DeviceIdType.MESH
f32 = jnp.float32
bf16 = jnp.bfloat16


def aligned(value, step):
    return pl.multiple_of(value, step)


def kernel(
    cfg,
    x_hbm,
    gate_hbm,
    up_hbm,
    down_hbm,
    value_hbm,
    glu_hbm,
    mix_hbm,
    gains_ref,
    small_ref,
    out_ref,
    *scratch,
):
    n_grp, n_fs, n_tp = cfg["n_grp"], cfg["n_fs"], cfg["n_tp"]
    R, E, DK, F, C, widths = cfg["R"], cfg["E"], cfg["DK"], cfg["F"], cfg["C"], cfg["widths"]
    D = E * n_tp
    n_x = n_tp // 2
    n_ch = R // LEN
    n_b = len(widths)
    scratch = list(scratch)
    take = lambda count: [scratch.pop(0) for _ in range(count)]
    gates, ups, downs = take(n_b), take(n_b), take(n_b)
    value_w, glu_w, mix_w = take(3)
    xfull, nbuf, acc, hbuf, pad_ref, conv_ref, gfull = take(7)
    rs1_s, rs1_r, rs2_s, rs2_r, st_s, st_r = take(6)
    sem_own, sem_x = take(2)
    recv_z, recv_y, send_r, send_l, send_y = take(5)
    ga_s, ga_r, ag_s, ag_r, s1_s, s1_r, s2_s, s2_r, ss_s, ss_r = take(10)

    g = lax.axis_index("grp")
    z = lax.axis_index("fs")
    tp = lax.axis_index("tp")
    xi = lax.div(tp, 2)
    par = lax.rem(tp, 2)
    partner = xi * 2 + 1 - par

    pieces = []
    start = 0
    for b, w in enumerate(widths):
        pieces.append((gates[b], gate_hbm.at[:, pl.ds(start, w)], "row"))
        pieces.append((ups[b], up_hbm.at[:, pl.ds(start, w)], "row"))
        pieces.append((downs[b], down_hbm.at[pl.ds(start, w), :], "col"))
        start += w
    pieces.append((value_w, value_hbm, "row"))
    pieces.append((glu_w, glu_hbm, "row"))
    pieces.append((mix_w, mix_hbm, "col"))
    n_p = len(pieces)

    def whole_of(p, src):
        ref, _, kind = pieces[p]
        if kind == "row":
            return ref.at[pl.ds(aligned(src * DK, DK), DK), :]
        return ref.at[src]

    def part_of(p, src, half):
        ref, _, kind = pieces[p]
        if kind == "row":
            size = DK // n_grp
            return ref.at[pl.ds(aligned(src * DK + half * size, size), size), :]
        size = ref.shape[1] // n_grp
        return ref.at[src, pl.ds(aligned(half * size, size), size), :]

    def own_copy(p):
        return pltpu.make_async_copy(pieces[p][1], whole_of(p, z), sem_own.at[p])

    def hop(p, src, sends, to):
        part = part_of(p, src, g)
        return pltpu.make_async_remote_copy(
            src_ref=part, dst_ref=part, send_sem=sends.at[p, src], recv_sem=recv_z.at[p, src],
            device_id={"fs": to}, device_id_type=MESH)

    def right(p, src):
        return hop(p, src, send_r, jnp.minimum(z + 1, n_fs - 1))

    def left(p, src):
        return hop(p, src, send_l, jnp.maximum(z - 1, 0))

    def across(p, src, step, half):
        part = part_of(p, src, half)
        return pltpu.make_async_remote_copy(
            src_ref=part, dst_ref=part, send_sem=send_y.at[p, src, step - 1],
            recv_sem=recv_y.at[p, src, step - 1],
            device_id={"grp": lax.rem(g + step, n_grp)}, device_id_type=MESH)

    def send_own(p):
        @pl.when(z < n_fs - 1)
        def _():
            right(p, z).start()

        @pl.when(z > 0)
        def _():
            left(p, z).start()

    def pump(p):
        def body(t, _):
            @pl.when(z - t >= 0)
            def _():
                src = jnp.maximum(z - t, 0)
                right(p, src).wait_recv()

                @pl.when(z < n_fs - 1)
                def _():
                    right(p, src).start()

                for step in range(1, n_grp):
                    across(p, src, step, g).start()

            @pl.when(z + t < n_fs)
            def _():
                src = jnp.minimum(z + t, n_fs - 1)
                left(p, src).wait_recv()

                @pl.when(z > 0)
                def _():
                    left(p, src).start()

                for step in range(1, n_grp):
                    across(p, src, step, g).start()

            return 0

        lax.fori_loop(1, n_fs, body, 0)

    def wait_across(p):
        def body(src, _):
            @pl.when(src != z)
            def _():
                for step in range(1, n_grp):
                    across(p, src, step, lax.rem(g + n_grp - step, n_grp)).wait_recv()

            return 0

        lax.fori_loop(0, n_fs, body, 0)

    def drain(p):
        def body(src, _):
            @pl.when((src <= z) & (z < n_fs - 1))
            def _():
                right(p, src).wait_send()

            @pl.when((src >= z) & (z > 0))
            def _():
                left(p, src).wait_send()

            @pl.when(src != z)
            def _():
                for step in range(1, n_grp):
                    across(p, src, step, g).wait_send()

            return 0

        lax.fori_loop(0, n_fs, body, 0)

    def rows_of(c):
        return pl.ds(aligned(c * LEN, LEN), LEN)

    def cols_of(t):
        return pl.ds(aligned(t * E, E), E)

    def gather(i, c, owner, to, slot):
        part = xfull.at[i, rows_of(c), cols_of(owner)]
        return pltpu.make_async_remote_copy(
            src_ref=part, dst_ref=part, send_sem=ag_s.at[i, c, slot], recv_sem=ag_r.at[i, c, owner],
            device_id={"tp": to}, device_id_type=MESH)

    def peer(d):
        return lax.rem(xi + d, n_x) * 2 + par

    def gather_send(i, c):
        for d in range(1, n_x):
            gather(i, c, tp, peer(d), d).start()
        gather(i, c, tp, partner, 0).start()

    def gather_forward(i, c):
        for d in range(1, n_x):
            src = lax.rem(xi + n_x - d, n_x) * 2 + par
            gather(i, c, src, tp, 0).wait_recv()
            gather(i, c, src, partner, n_x + d - 1).start()

    def gather_wait(i, c):
        for j in range(n_x):
            gather(i, c, j * 2 + 1 - par, tp, 0).wait_recv()

    def gather_drain(i, c):
        for slot in range(2 * n_x - 1):
            gather(i, c, tp, partner, slot).wait_send()

    def pair(i, c):
        return pltpu.make_async_remote_copy(
            src_ref=rs1_s.at[i, :, rows_of(c), :], dst_ref=rs1_r.at[i, :, rows_of(c), :],
            send_sem=s1_s.at[i, c], recv_sem=s1_r.at[i, c],
            device_id={"tp": partner}, device_id_type=MESH)

    def cross(i, c, d):
        return pltpu.make_async_remote_copy(
            src_ref=rs2_s.at[i, d - 1, rows_of(c), :], dst_ref=rs2_r.at[i, d - 1, rows_of(c), :],
            send_sem=s2_s.at[i, c, d - 1], recv_sem=s2_r.at[i, c, d - 1],
            device_id={"tp": peer(d)}, device_id_type=MESH)

    def sum_start(i, c):
        for j in range(n_x):
            rs1_s[i, j, rows_of(c), :] = acc[rows_of(c), cols_of(j * 2 + 1 - par)].astype(bf16)
        pair(i, c).start()

    def sum_cross(i, c):
        pair(i, c).wait_recv()
        for d in range(1, n_x):
            j = lax.rem(xi + d, n_x)
            rs2_s[i, d - 1, rows_of(c), :] = (
                acc[rows_of(c), cols_of(j * 2 + par)] + rs1_r[i, j, rows_of(c), :].astype(f32)
            ).astype(bf16)
            cross(i, c, d).start()

    def sum_end(i, c):
        total = acc[rows_of(c), cols_of(tp)] + rs1_r[i, xi, rows_of(c), :].astype(f32)
        for d in range(1, n_x):
            cross(i, c, d).wait_recv()
            total = total + rs2_r[i, d - 1, rows_of(c), :].astype(f32)
        return total

    def each(body):
        def step(c, _):
            body(c)
            return 0

        lax.fori_loop(0, n_ch, step, 0)

    def norm(i, c):
        def body(k, _):
            rows = pl.ds(aligned(c * LEN + k * SUB, SUB), SUB)
            values = xfull[i, rows, :].astype(f32)
            inverse = lax.rsqrt(jnp.sum(values * values, axis=1, keepdims=True) / D + epsilon)
            nbuf[rows, :] = (values * inverse * gfull[pl.ds(i, 1), :]).astype(bf16)
            return 0

        lax.fori_loop(0, LEN // SUB, body, 0)

    def hidden_of(b, c):
        rows = nbuf[rows_of(c), :]
        gate = jnp.dot(rows, gates[b][...], preferred_element_type=f32)
        up = jnp.dot(rows, ups[b][...], preferred_element_type=f32)
        return (gate * jax.nn.sigmoid(gate) * up).astype(bf16)

    barrier = pltpu.get_barrier_semaphore()
    for step in (1, n_fs - 1):
        pl.semaphore_signal(barrier, inc=1, device_id={"fs": lax.rem(z + step, n_fs)}, device_id_type=MESH)
    for step in range(1, n_grp):
        pl.semaphore_signal(barrier, inc=1, device_id={"grp": lax.rem(g + step, n_grp)}, device_id_type=MESH)
    for step in range(1, n_tp):
        pl.semaphore_signal(barrier, inc=1, device_id={"tp": lax.rem(tp + step, n_tp)}, device_id_type=MESH)
    x_copy = pltpu.make_async_copy(x_hbm, xfull.at[0, :, cols_of(tp)], sem_x)
    for p in range(n_p):
        own_copy(p).start()
        if p == LEAD - 1:
            x_copy.start()
    gfull[:, cols_of(tp)] = gains_ref[...]
    pad_ref[pl.ds(0, 32), :] = jnp.zeros((32, C), f32)
    pl.semaphore_wait(barrier, 2 + n_grp - 1 + n_tp - 1)

    def gain_copy(owner, step):
        return pltpu.make_async_remote_copy(
            src_ref=gains_ref, dst_ref=gfull.at[:, cols_of(owner)], send_sem=ga_s.at[step - 1],
            recv_sem=ga_r.at[step - 1], device_id={"tp": lax.rem(tp + step, n_tp)}, device_id_type=MESH)

    for p in range(LEAD):
        own_copy(p).wait()
        send_own(p)
    x_copy.wait()
    each(lambda c: gather_send(0, c))
    for step in range(1, n_tp):
        gain_copy(tp, step).start()
    for p in range(LEAD, n_p):
        own_copy(p).wait()

    queue = []

    def unit(b):
        def run(c):
            hidden = hidden_of(b, c)
            for s in range(n_fs):
                columns = pl.ds(s * downs[b].shape[2], downs[b].shape[2])
                part = jnp.dot(hidden, downs[b][s], preferred_element_type=f32)
                if b == 0:
                    acc[rows_of(c), columns] = part
                else:
                    acc[rows_of(c), columns] += part
        return run

    done = 0
    for p in range(n_p):
        if p + LEAD < n_p:
            send_own(p + LEAD)
        pump(p)
        if p == 0:
            each(lambda c: gather_forward(0, c))
            for step in range(1, n_tp):
                gain_copy(tp, step).wait_recv()
        if p == 1:
            each(lambda c: gather_wait(0, c))
            each(lambda c: norm(0, c))
        if p >= 1 and p - 1 < 3 * n_b:
            wait_across(p - 1)
            if (p - 1) % 3 == 2:
                b = (p - 1) // 3
                each(unit(b))
                if b == n_b - 1:
                    each(lambda c: sum_start(0, c))
    each(lambda c: sum_cross(0, c))

    def close(i, scale):
        def run(c):
            total = sum_end(i, c)
            fresh = xfull[i, rows_of(c), cols_of(tp)].astype(f32) + scale * total
            xfull[i + 1, rows_of(c), cols_of(tp)] = fresh.astype(bf16)
            gather_send(i + 1, c)
        return run

    each(close(0, 0.5))
    for p in range(3 * n_b, n_p):
        wait_across(p)
    each(lambda c: gather_forward(1, c))

    def stat_copy(c, step):
        return pltpu.make_async_remote_copy(
            src_ref=st_s.at[c], dst_ref=st_r.at[c, step - 1], send_sem=ss_s.at[c, step - 1],
            recv_sem=ss_r.at[c, step - 1], device_id={"tp": lax.rem(tp + step, n_tp)}, device_id_type=MESH)

    def conv_front(c):
        gather_wait(1, c)
        norm(1, c)
        rows = nbuf[rows_of(c), :]
        value = jnp.dot(rows, value_w[...], preferred_element_type=f32)
        gating = jnp.dot(rows, glu_w[...], preferred_element_type=f32)
        pad_ref[pl.ds(32, LEN), :] = value * jax.nn.sigmoid(gating)
        total = jnp.zeros((LEN, C), f32)
        for k in range(KERNEL):
            total = total + small_ref[pl.ds(k, 1), :] * pad_ref[pl.ds(33 - KERNEL + k, LEN), :]
        conv_ref[rows_of(c), :] = total
        lanes = lax.broadcasted_iota(jnp.int32, (LEN, 128), 1)
        both = jnp.where(lanes == 0, jnp.sum(total, axis=1, keepdims=True),
                         jnp.sum(total * total, axis=1, keepdims=True))
        st_s[c] = jnp.transpose(both)[0:8, :]
        for step in range(1, n_tp):
            stat_copy(c, step).start()

    each(conv_front)

    def conv_back(c):
        stats = st_s[c]
        for step in range(1, n_tp):
            stat_copy(c, step).wait_recv()
            stats = stats + st_r[c, step - 1]
        stats = jnp.concatenate([stats, jnp.zeros((LEN - 8, LEN), f32)], axis=0)
        turned = jnp.transpose(stats)
        mean = turned[:, 0:1] / (C * n_tp)
        spread = turned[:, 1:2] / (C * n_tp) - mean * mean
        normed = (conv_ref[rows_of(c), :] - mean) * lax.rsqrt(spread + epsilon) * small_ref[
            pl.ds(KERNEL, 1), :] + small_ref[pl.ds(KERNEL + 1, 1), :]
        mixed = (normed * jax.nn.sigmoid(normed)).astype(bf16)
        for s in range(n_fs):
            acc[rows_of(c), pl.ds(s * mix_w.shape[2], mix_w.shape[2])] = jnp.dot(
                mixed, mix_w[s], preferred_element_type=f32)
        sum_start(1, c)

    each(conv_back)
    each(lambda c: sum_cross(1, c))
    each(close(1, 1.0))
    each(lambda c: gather_forward(2, c))

    def second(c):
        gather_wait(2, c)
        norm(2, c)
        start = 0
        for b, w in enumerate(widths):
            hbuf[:, pl.ds(start, w)] = hidden_of(b, c)
            start += w

        @pl.when(c > 0)
        def _():
            sum_cross(2, jnp.maximum(c - 1, 0))

        for s in range(n_fs):
            start = 0
            part = jnp.zeros((LEN, downs[0].shape[2]), f32)
            for b, w in enumerate(widths):
                part = part + jnp.dot(hbuf[:, pl.ds(start, w)], downs[b][s], preferred_element_type=f32)
                start += w
            acc[rows_of(c), pl.ds(s * downs[0].shape[2], downs[0].shape[2])] = part
        sum_start(2, c)

    each(second)
    sum_cross(2, n_ch - 1)

    def last(c):
        total = sum_end(2, c)
        out_ref[rows_of(c), :] = (xfull[2, rows_of(c), cols_of(tp)].astype(f32) + 0.5 * total).astype(bf16)

    each(last)

    for p in range(n_p):
        drain(p)
    for step in range(1, n_tp):
        gain_copy(tp, step).wait_send()

    def leave(c):
        for i in range(3):
            gather_drain(i, c)
            pair(i, c).wait_send()
            for d in range(1, n_x):
                cross(i, c, d).wait_send()
        for step in range(1, n_tp):
            stat_copy(c, step).wait_send()

    each(leave)


def solution(mesh):
    n_grp, n_fs, n_tp = mesh.shape["grp"], mesh.shape["fs"], mesh.shape["tp"]

    def local(
        stream_in, gain_before, gain_mixer, gain_after, w_gate, w_upward, w_down, w_value,
        w_glu_gate, conv_taps, chan_gain, chan_bias, w_mix_out,
    ):
        R, E = stream_in.shape
        DK, F = w_gate.shape
        C = w_value.shape[1]
        E2 = w_down.shape[1]
        D = E * n_tp
        n_x, n_ch = n_tp // 2, R // LEN
        widths = [min(WIDE, F - start) for start in range(0, F, WIDE)]
        cfg = dict(n_grp=n_grp, n_fs=n_fs, n_tp=n_tp, R=R, E=E, DK=DK, F=F, C=C, widths=widths)
        gains = jnp.concatenate(
            [gain_before[None], gain_mixer[None], gain_after[None], jnp.zeros((5, E), bf16)], axis=0
        ).astype(f32)
        small = jnp.concatenate(
            [conv_taps, chan_gain[None], chan_bias[None], jnp.zeros((7, C), bf16)], axis=0
        ).astype(f32)
        n_p = 3 * len(widths) + 3
        dma = pltpu.SemaphoreType.DMA
        scratch = [pltpu.VMEM((D, w), bf16) for w in widths] * 2
        scratch += [pltpu.VMEM((n_fs, w, E2), bf16) for w in widths]
        scratch += [pltpu.VMEM((D, C), bf16)] * 2 + [pltpu.VMEM((n_fs, C, E2), bf16)]
        scratch += [
            pltpu.VMEM((3, R, D), bf16), pltpu.VMEM((R, D), bf16), pltpu.VMEM((R, D), f32),
            pltpu.VMEM((LEN, F), bf16), pltpu.VMEM((32 + LEN, C), f32), pltpu.VMEM((R, C), f32),
            pltpu.VMEM((8, D), f32),
            pltpu.VMEM((3, n_x, R, E), bf16), pltpu.VMEM((3, n_x, R, E), bf16),
            pltpu.VMEM((3, n_x - 1, R, E), bf16), pltpu.VMEM((3, n_x - 1, R, E), bf16),
            pltpu.VMEM((n_ch, 8, LEN), f32), pltpu.VMEM((n_ch, n_tp - 1, 8, LEN), f32),
            dma((n_p,)), dma,
            dma((n_p, n_fs)), dma((n_p, n_fs, n_grp - 1)), dma((n_p, n_fs)), dma((n_p, n_fs)),
            dma((n_p, n_fs, n_grp - 1)),
            dma((n_tp - 1,)), dma((n_tp - 1,)),
            dma((3, n_ch, 2 * n_x - 1)), dma((3, n_ch, n_tp)),
            dma((3, n_ch)), dma((3, n_ch)),
            dma((3, n_ch, n_x - 1)), dma((3, n_ch, n_x - 1)),
            dma((n_ch, n_tp - 1)), dma((n_ch, n_tp - 1)),
        ]
        hbm = pl.BlockSpec(memory_space=pl.ANY)
        vmem = pl.BlockSpec(memory_space=pltpu.VMEM)
        return pl.pallas_call(
            functools.partial(kernel, cfg),
            out_shape=jax.ShapeDtypeStruct((R, E), bf16),
            in_specs=[hbm] * 7 + [vmem] * 2,
            out_specs=vmem,
            scratch_shapes=scratch,
            compiler_params=pltpu.CompilerParams(
                collective_id=0, has_side_effects=True, vmem_limit_bytes=62 * 1024 * 1024),
        )(stream_in, w_gate, w_upward, w_down, w_value, w_glu_gate, w_mix_out, gains, small)

    in_specs = (
        P(("grp", "fs"), "tp"), P("tp"), P("tp"), P("tp"), P("fs", "tp"), P("fs", "tp"),
        P("tp", "fs"), P("fs", "tp"), P("fs", "tp"), P(None, "tp"), P("tp"), P("tp"), P("tp", "fs"),
    )
    return jax.shard_map(
        local, mesh=mesh, in_specs=in_specs, out_specs=P(("grp", "fs"), "tp"), check_vma=False)
```

```python
import functools

import jax
import jax.numpy as jnp
from jax import lax
from jax.experimental import pallas as pl
from jax.experimental.pallas import tpu as pltpu
from jax.sharding import PartitionSpec as P

KERNEL = 31
LEN = 128
WIDE = 384
LEAD = 1
LAG = 1
SUB = 64

epsilon = 1e-06
MESH = pl.DeviceIdType.MESH
f32 = jnp.float32
bf16 = jnp.bfloat16


def aligned(value, step):
    return pl.multiple_of(value, step)


def kernel(
    cfg,
    x_hbm,
    gate_hbm,
    up_hbm,
    down_hbm,
    value_hbm,
    glu_hbm,
    mix_hbm,
    gains_ref,
    small_ref,
    out_ref,
    *scratch,
):
    n_grp, n_fs, n_tp = cfg["n_grp"], cfg["n_fs"], cfg["n_tp"]
    R, E, DK, F, C, widths = cfg["R"], cfg["E"], cfg["DK"], cfg["F"], cfg["C"], cfg["widths"]
    D = E * n_tp
    n_x = n_tp // 2
    n_ch = R // LEN
    n_b = len(widths)
    scratch = list(scratch)
    take = lambda count: [scratch.pop(0) for _ in range(count)]
    gates, ups, downs = take(n_b), take(n_b), take(n_b)
    value_w, glu_w, mix_w = take(3)
    xfull, nbuf, acc, hbuf, pad_ref, conv_ref, gfull = take(7)
    rs1_s, rs1_r, rs2_s, rs2_r, st_s, st_r = take(6)
    sem_own, sem_x = take(2)
    recv_z, recv_y, send_r, send_l, send_y = take(5)
    ga_s, ga_r, ag_s, ag_r, s1_s, s1_r, s2_s, s2_r, ss_s, ss_r = take(10)

    g = lax.axis_index("grp")
    z = lax.axis_index("fs")
    tp = lax.axis_index("tp")
    xi = lax.div(tp, 2)
    par = lax.rem(tp, 2)
    partner = xi * 2 + 1 - par

    pieces = []
    start = 0
    for b, w in enumerate(widths):
        pieces.append((gates[b], gate_hbm.at[:, pl.ds(start, w)], "row"))
        pieces.append((ups[b], up_hbm.at[:, pl.ds(start, w)], "row"))
        pieces.append((downs[b], down_hbm.at[pl.ds(start, w), :], "col"))
        start += w
    pieces.append((value_w, value_hbm, "row"))
    pieces.append((glu_w, glu_hbm, "row"))
    pieces.append((mix_w, mix_hbm, "col"))
    n_p = len(pieces)

    def whole_of(p, src):
        ref, _, kind = pieces[p]
        if kind == "row":
            return ref.at[pl.ds(aligned(src * DK, DK), DK), :]
        return ref.at[src]

    def part_of(p, src, half):
        ref, _, kind = pieces[p]
        if kind == "row":
            size = DK // n_grp
            return ref.at[pl.ds(aligned(src * DK + half * size, size), size), :]
        size = ref.shape[1] // n_grp
        return ref.at[src, pl.ds(aligned(half * size, size), size), :]

    def own_copy(p):
        return pltpu.make_async_copy(pieces[p][1], whole_of(p, z), sem_own.at[p])

    def hop(p, src, sends, to):
        part = part_of(p, src, g)
        return pltpu.make_async_remote_copy(
            src_ref=part, dst_ref=part, send_sem=sends.at[p, src], recv_sem=recv_z.at[p, src],
            device_id={"fs": to}, device_id_type=MESH)

    def right(p, src):
        return hop(p, src, send_r, jnp.minimum(z + 1, n_fs - 1))

    def left(p, src):
        return hop(p, src, send_l, jnp.maximum(z - 1, 0))

    def across(p, src, step, half):
        part = part_of(p, src, half)
        return pltpu.make_async_remote_copy(
            src_ref=part, dst_ref=part, send_sem=send_y.at[p, src, step - 1],
            recv_sem=recv_y.at[p, src, step - 1],
            device_id={"grp": lax.rem(g + step, n_grp)}, device_id_type=MESH)

    def send_own(p):
        @pl.when(z < n_fs - 1)
        def _():
            right(p, z).start()

        @pl.when(z > 0)
        def _():
            left(p, z).start()

    def pump(p, t):
        @pl.when(z - t >= 0)
        def _():
            src = jnp.maximum(z - t, 0)
            right(p, src).wait_recv()

            @pl.when(z < n_fs - 1)
            def _():
                right(p, src).start()

            for step in range(1, n_grp):
                across(p, src, step, g).start()

        @pl.when(z + t < n_fs)
        def _():
            src = jnp.minimum(z + t, n_fs - 1)
            left(p, src).wait_recv()

            @pl.when(z > 0)
            def _():
                left(p, src).start()

            for step in range(1, n_grp):
                across(p, src, step, g).start()

    def wait_across(p):
        def body(src, _):
            @pl.when(src != z)
            def _():
                for step in range(1, n_grp):
                    across(p, src, step, lax.rem(g + n_grp - step, n_grp)).wait_recv()

            return 0

        lax.fori_loop(0, n_fs, body, 0)

    def drain(p):
        def body(src, _):
            @pl.when((src <= z) & (z < n_fs - 1))
            def _():
                right(p, src).wait_send()

            @pl.when((src >= z) & (z > 0))
            def _():
                left(p, src).wait_send()

            @pl.when(src != z)
            def _():
                for step in range(1, n_grp):
                    across(p, src, step, g).wait_send()

            return 0

        lax.fori_loop(0, n_fs, body, 0)

    def rows_of(c):
        return pl.ds(aligned(c * LEN, LEN), LEN)

    def cols_of(t):
        return pl.ds(aligned(t * E, E), E)

    def gather(i, c, owner, to, slot):
        part = xfull.at[i, rows_of(c), cols_of(owner)]
        return pltpu.make_async_remote_copy(
            src_ref=part, dst_ref=part, send_sem=ag_s.at[i, c, slot], recv_sem=ag_r.at[i, c, owner],
            device_id={"tp": to}, device_id_type=MESH)

    def peer(d):
        return lax.rem(xi + d, n_x) * 2 + par

    def gather_send(i, c):
        for d in range(1, n_x):
            gather(i, c, tp, peer(d), d).start()
        gather(i, c, tp, partner, 0).start()

    def gather_forward(i, c):
        for d in range(1, n_x):
            src = lax.rem(xi + n_x - d, n_x) * 2 + par
            gather(i, c, src, tp, 0).wait_recv()
            gather(i, c, src, partner, n_x + d - 1).start()

    def gather_wait(i, c):
        for j in range(n_x):
            gather(i, c, j * 2 + 1 - par, tp, 0).wait_recv()

    def gather_drain(i, c):
        for slot in range(2 * n_x - 1):
            gather(i, c, tp, partner, slot).wait_send()

    def pair(i, c):
        return pltpu.make_async_remote_copy(
            src_ref=rs1_s.at[i, :, rows_of(c), :], dst_ref=rs1_r.at[i, :, rows_of(c), :],
            send_sem=s1_s.at[i, c], recv_sem=s1_r.at[i, c],
            device_id={"tp": partner}, device_id_type=MESH)

    def cross(i, c, d):
        return pltpu.make_async_remote_copy(
            src_ref=rs2_s.at[i, d - 1, rows_of(c), :], dst_ref=rs2_r.at[i, d - 1, rows_of(c), :],
            send_sem=s2_s.at[i, c, d - 1], recv_sem=s2_r.at[i, c, d - 1],
            device_id={"tp": peer(d)}, device_id_type=MESH)

    def sum_start(i, c):
        for j in range(n_x):
            rs1_s[i, j, rows_of(c), :] = acc[rows_of(c), cols_of(j * 2 + 1 - par)].astype(bf16)
        pair(i, c).start()

    def sum_cross(i, c):
        pair(i, c).wait_recv()
        for d in range(1, n_x):
            j = lax.rem(xi + d, n_x)
            rs2_s[i, d - 1, rows_of(c), :] = (
                acc[rows_of(c), cols_of(j * 2 + par)] + rs1_r[i, j, rows_of(c), :].astype(f32)
            ).astype(bf16)
            cross(i, c, d).start()

    def sum_end(i, c):
        total = acc[rows_of(c), cols_of(tp)] + rs1_r[i, xi, rows_of(c), :].astype(f32)
        for d in range(1, n_x):
            cross(i, c, d).wait_recv()
            total = total + rs2_r[i, d - 1, rows_of(c), :].astype(f32)
        return total

    def each(body):
        def step(c, _):
            body(c)
            return 0

        lax.fori_loop(0, n_ch, step, 0)

    def norm(i, c):
        def body(k, _):
            rows = pl.ds(aligned(c * LEN + k * SUB, SUB), SUB)
            values = xfull[i, rows, :].astype(f32)
            inverse = lax.rsqrt(jnp.sum(values * values, axis=1, keepdims=True) / D + epsilon)
            nbuf[rows, :] = (values * inverse * gfull[pl.ds(i, 1), :]).astype(bf16)
            return 0

        lax.fori_loop(0, LEN // SUB, body, 0)

    def hidden_of(b, c):
        rows = nbuf[rows_of(c), :]
        gate = jnp.dot(rows, gates[b][...], preferred_element_type=f32)
        up = jnp.dot(rows, ups[b][...], preferred_element_type=f32)
        return (gate * jax.nn.sigmoid(gate) * up).astype(bf16)

    barrier = pltpu.get_barrier_semaphore()
    for step in (1, n_fs - 1):
        pl.semaphore_signal(barrier, inc=1, device_id={"fs": lax.rem(z + step, n_fs)}, device_id_type=MESH)
    for step in range(1, n_grp):
        pl.semaphore_signal(barrier, inc=1, device_id={"grp": lax.rem(g + step, n_grp)}, device_id_type=MESH)
    for step in range(1, n_tp):
        pl.semaphore_signal(barrier, inc=1, device_id={"tp": lax.rem(tp + step, n_tp)}, device_id_type=MESH)
    x_copy = pltpu.make_async_copy(x_hbm, xfull.at[0, :, cols_of(tp)], sem_x)
    for p in range(n_p):
        own_copy(p).start()
        if p == LEAD - 1:
            x_copy.start()
    gfull[:, cols_of(tp)] = gains_ref[...]
    pad_ref[pl.ds(0, 32), :] = jnp.zeros((32, C), f32)
    pl.semaphore_wait(barrier, 2 + n_grp - 1 + n_tp - 1)

    def gain_copy(owner, step):
        return pltpu.make_async_remote_copy(
            src_ref=gains_ref, dst_ref=gfull.at[:, cols_of(owner)], send_sem=ga_s.at[step - 1],
            recv_sem=ga_r.at[step - 1], device_id={"tp": lax.rem(tp + step, n_tp)}, device_id_type=MESH)

    for p in range(LEAD):
        own_copy(p).wait()
        send_own(p)
    x_copy.wait()
    each(lambda c: gather_send(0, c))
    for step in range(1, n_tp):
        gain_copy(tp, step).start()
    for p in range(LEAD, n_p):
        own_copy(p).wait()

    def unit(b):
        def run(c):
            hidden = hidden_of(b, c)
            for s in range(n_fs):
                columns = pl.ds(s * downs[b].shape[2], downs[b].shape[2])
                part = jnp.dot(hidden, downs[b][s], preferred_element_type=f32)
                if b == 0:
                    acc[rows_of(c), columns] = part
                else:
                    acc[rows_of(c), columns] += part
        return run

    def close(i, scale):
        def run(c):
            total = sum_end(i, c)
            fresh = xfull[i, rows_of(c), cols_of(tp)].astype(f32) + scale * total
            xfull[i + 1, rows_of(c), cols_of(tp)] = fresh.astype(bf16)
            gather_send(i + 1, c)
        return run

    after = [
        lambda: each(lambda c: sum_cross(0, c)),
        lambda: each(close(0, 0.5)),
    ]
    ended = False
    for k in range(n_p + n_fs - 2):
        if k + LEAD < n_p:
            send_own(k + LEAD)
        for t in range(1, n_fs):
            if 0 <= k - (t - 1) < n_p:
                pump(k - (t - 1), t)
        if ended and after:
            after.pop(0)()
        if k == 0:
            each(lambda c: gather_forward(0, c))
            for step in range(1, n_tp):
                gain_copy(tp, step).wait_recv()
        if k == 1:
            each(lambda c: gather_wait(0, c))
            each(lambda c: norm(0, c))
        q = k - (n_fs - 2) - LAG
        if 0 <= q < 3 * n_b:
            wait_across(q)
            if q % 3 == 2:
                each(unit(q // 3))
            if q == 3 * n_b - 1:
                each(lambda c: sum_start(0, c))
                ended = True
    for stage in after:
        stage()
    for p in range(3 * n_b, n_p):
        wait_across(p)
    each(lambda c: gather_forward(1, c))

    def stat_copy(c, step):
        return pltpu.make_async_remote_copy(
            src_ref=st_s.at[c], dst_ref=st_r.at[c, step - 1], send_sem=ss_s.at[c, step - 1],
            recv_sem=ss_r.at[c, step - 1], device_id={"tp": lax.rem(tp + step, n_tp)}, device_id_type=MESH)

    def conv_front(c):
        gather_wait(1, c)
        norm(1, c)
        rows = nbuf[rows_of(c), :]
        value = jnp.dot(rows, value_w[...], preferred_element_type=f32)
        gating = jnp.dot(rows, glu_w[...], preferred_element_type=f32)
        pad_ref[pl.ds(32, LEN), :] = value * jax.nn.sigmoid(gating)
        total = jnp.zeros((LEN, C), f32)
        for k in range(KERNEL):
            total = total + small_ref[pl.ds(k, 1), :] * pad_ref[pl.ds(33 - KERNEL + k, LEN), :]
        conv_ref[rows_of(c), :] = total
        lanes = lax.broadcasted_iota(jnp.int32, (LEN, 128), 1)
        both = jnp.where(lanes == 0, jnp.sum(total, axis=1, keepdims=True),
                         jnp.sum(total * total, axis=1, keepdims=True))
        st_s[c] = jnp.transpose(both)[0:8, :]
        for step in range(1, n_tp):
            stat_copy(c, step).start()

    each(conv_front)

    def conv_back(c):
        stats = st_s[c]
        for step in range(1, n_tp):
            stat_copy(c, step).wait_recv()
            stats = stats + st_r[c, step - 1]
        stats = jnp.concatenate([stats, jnp.zeros((LEN - 8, LEN), f32)], axis=0)
        turned = jnp.transpose(stats)
        mean = turned[:, 0:1] / (C * n_tp)
        spread = turned[:, 1:2] / (C * n_tp) - mean * mean
        normed = (conv_ref[rows_of(c), :] - mean) * lax.rsqrt(spread + epsilon) * small_ref[
            pl.ds(KERNEL, 1), :] + small_ref[pl.ds(KERNEL + 1, 1), :]
        mixed = (normed * jax.nn.sigmoid(normed)).astype(bf16)
        for s in range(n_fs):
            acc[rows_of(c), pl.ds(s * mix_w.shape[2], mix_w.shape[2])] = jnp.dot(
                mixed, mix_w[s], preferred_element_type=f32)
        sum_start(1, c)

    each(conv_back)
    each(lambda c: sum_cross(1, c))
    each(close(1, 1.0))
    each(lambda c: gather_forward(2, c))

    def second(c):
        gather_wait(2, c)
        norm(2, c)
        start = 0
        for b, w in enumerate(widths):
            hbuf[:, pl.ds(start, w)] = hidden_of(b, c)
            start += w

        @pl.when(c > 0)
        def _():
            sum_cross(2, jnp.maximum(c - 1, 0))

        for s in range(n_fs):
            start = 0
            part = jnp.zeros((LEN, downs[0].shape[2]), f32)
            for b, w in enumerate(widths):
                part = part + jnp.dot(hbuf[:, pl.ds(start, w)], downs[b][s], preferred_element_type=f32)
                start += w
            acc[rows_of(c), pl.ds(s * downs[0].shape[2], downs[0].shape[2])] = part
        sum_start(2, c)

    each(second)
    sum_cross(2, n_ch - 1)

    def last(c):
        total = sum_end(2, c)
        out_ref[rows_of(c), :] = (xfull[2, rows_of(c), cols_of(tp)].astype(f32) + 0.5 * total).astype(bf16)

    each(last)

    for p in range(n_p):
        drain(p)
    for step in range(1, n_tp):
        gain_copy(tp, step).wait_send()

    def leave(c):
        for i in range(3):
            gather_drain(i, c)
            pair(i, c).wait_send()
            for d in range(1, n_x):
                cross(i, c, d).wait_send()
        for step in range(1, n_tp):
            stat_copy(c, step).wait_send()

    each(leave)


def solution(mesh):
    n_grp, n_fs, n_tp = mesh.shape["grp"], mesh.shape["fs"], mesh.shape["tp"]

    def local(
        stream_in, gain_before, gain_mixer, gain_after, w_gate, w_upward, w_down, w_value,
        w_glu_gate, conv_taps, chan_gain, chan_bias, w_mix_out,
    ):
        R, E = stream_in.shape
        DK, F = w_gate.shape
        C = w_value.shape[1]
        E2 = w_down.shape[1]
        D = E * n_tp
        n_x, n_ch = n_tp // 2, R // LEN
        widths = [min(WIDE, F - start) for start in range(0, F, WIDE)]
        cfg = dict(n_grp=n_grp, n_fs=n_fs, n_tp=n_tp, R=R, E=E, DK=DK, F=F, C=C, widths=widths)
        gains = jnp.concatenate(
            [gain_before[None], gain_mixer[None], gain_after[None], jnp.zeros((5, E), bf16)], axis=0
        ).astype(f32)
        small = jnp.concatenate(
            [conv_taps, chan_gain[None], chan_bias[None], jnp.zeros((7, C), bf16)], axis=0
        ).astype(f32)
        n_p = 3 * len(widths) + 3
        dma = pltpu.SemaphoreType.DMA
        scratch = [pltpu.VMEM((D, w), bf16) for w in widths] * 2
        scratch += [pltpu.VMEM((n_fs, w, E2), bf16) for w in widths]
        scratch += [pltpu.VMEM((D, C), bf16)] * 2 + [pltpu.VMEM((n_fs, C, E2), bf16)]
        scratch += [
            pltpu.VMEM((3, R, D), bf16), pltpu.VMEM((R, D), bf16), pltpu.VMEM((R, D), f32),
            pltpu.VMEM((LEN, F), bf16), pltpu.VMEM((32 + LEN, C), f32), pltpu.VMEM((R, C), f32),
            pltpu.VMEM((8, D), f32),
            pltpu.VMEM((3, n_x, R, E), bf16), pltpu.VMEM((3, n_x, R, E), bf16),
            pltpu.VMEM((3, n_x - 1, R, E), bf16), pltpu.VMEM((3, n_x - 1, R, E), bf16),
            pltpu.VMEM((n_ch, 8, LEN), f32), pltpu.VMEM((n_ch, n_tp - 1, 8, LEN), f32),
            dma((n_p,)), dma,
            dma((n_p, n_fs)), dma((n_p, n_fs, n_grp - 1)), dma((n_p, n_fs)), dma((n_p, n_fs)),
            dma((n_p, n_fs, n_grp - 1)),
            dma((n_tp - 1,)), dma((n_tp - 1,)),
            dma((3, n_ch, 2 * n_x - 1)), dma((3, n_ch, n_tp)),
            dma((3, n_ch)), dma((3, n_ch)),
            dma((3, n_ch, n_x - 1)), dma((3, n_ch, n_x - 1)),
            dma((n_ch, n_tp - 1)), dma((n_ch, n_tp - 1)),
        ]
        hbm = pl.BlockSpec(memory_space=pl.ANY)
        vmem = pl.BlockSpec(memory_space=pltpu.VMEM)
        return pl.pallas_call(
            functools.partial(kernel, cfg),
            out_shape=jax.ShapeDtypeStruct((R, E), bf16),
            in_specs=[hbm] * 7 + [vmem] * 2,
            out_specs=vmem,
            scratch_shapes=scratch,
            compiler_params=pltpu.CompilerParams(
                collective_id=0, has_side_effects=True, vmem_limit_bytes=62 * 1024 * 1024),
        )(stream_in, w_gate, w_upward, w_down, w_value, w_glu_gate, w_mix_out, gains, small)

    in_specs = (
        P(("grp", "fs"), "tp"), P("tp"), P("tp"), P("tp"), P("fs", "tp"), P("fs", "tp"),
        P("tp", "fs"), P("fs", "tp"), P("fs", "tp"), P(None, "tp"), P("tp"), P("tp"), P("tp", "fs"),
    )
    return jax.shard_map(
        local, mesh=mesh, in_specs=in_specs, out_specs=P(("grp", "fs"), "tp"), check_vma=False)
```
